32 devices in a mesh: sp: 16 (over z, y, core), tp: 2 (over x).
Axes of the slice: x: 2, y: 2, z: 4, core: 2. Of those that a mesh axis runs over, the one named last changes fastest.
Arguments:
- queries: bfloat16 [16384, 1024], P('sp', 'tp'), may hold values from -8 to 8
- keys: bfloat16 [16384, 256], P('sp', 'tp'), may hold values from -8 to 8
- values: bfloat16 [16384, 256], P('sp', 'tp'), may hold values from -18 to 18
- doc_ids: int32 [16384], P('sp'), may hold values from 0 to 3, never falling along the last dimension, each value on 1 to 8192 neighbouring positions
- sinks: float32 [16], P('tp'), may hold values from 0 to 4
- residual: bfloat16 [16384, 2048], P(('sp', 'tp')), may hold values from -12 to 12
- out_weight: bfloat16 [1024, 2048], P('tp'), may hold values from -0.1875 to 0.1875
- norm_gain: float32 [2048], replicated, may hold values from 0.1 to 1.9
- w_gate: bfloat16 [2048, 5632], P('sp', 'tp'), may hold values from -0.125 to 0.125
- w_value: bfloat16 [2048, 5632], P('sp', 'tp'), may hold values from -0.125 to 0.125
- conv_gate: float32 [3, 5632], P(None, 'tp'), may hold values from -3.5 to 3.5
- conv_value: float32 [3, 5632], P(None, 'tp'), may hold values from -3.5 to 3.5
- w_down: bfloat16 [5632, 2048], P('tp', 'sp'), may hold values from -0.078125 to 0.078125
Outputs:
- layer_out: bfloat16 [16384, 2048], P(('sp', 'tp'))
The draws below stay inside these ranges and needn't reach their ends.
All inputs are finite; a program needn't handle non-finite values.
Results may differ from the reference program's by a relative error of at most 0.012.
Values may be sent and summed in bfloat16 or wider, within the bound.
No kernel may reach another device: no remote copies, remote signals or barrier semaphores. Data moves between devices by JAX's collectives and lax.ppermute only.
A program may use at most 128 MiB of HBM per device.

```python
import math
import jax
import jax.numpy as jnp
import numpy as np
from jax import lax

D = 2048
HEAD_DIM = 64
A_HEADS = 16
FF = 5632
WINDOW = 128
TOK_SP = 1024
TOKENS = 16384
A_Q = 1024
KV_W = 256
DOCS = 4
N_SP = 16


def draw_keys(key, part):
    base = jnp.clip(jax.random.normal(jax.random.fold_in(key, 1), (TOKENS, KV_W), jnp.float32), -8.0, 8.0)
    return base.astype(jnp.bfloat16)


def draw_queries(key, part):
    base = jnp.clip(jax.random.normal(jax.random.fold_in(key, 2), (TOKENS, A_Q), jnp.float32), -8.0, 8.0)
    return base.astype(jnp.bfloat16)


def draw_residual(key, part):
    base = jax.random.normal(jax.random.fold_in(key, 3), (TOKENS, D), jnp.float32)
    spread = jax.random.uniform(jax.random.fold_in(key, 4), (TOKENS, 1), jnp.float32, math.log(1.0 / 3.0), math.log(3.0))
    base = base * jnp.exp(spread)
    return jnp.clip(base, -12.0, 12.0).astype(jnp.bfloat16)


def shard_levels(key, shape, shards, least, top_value):
    gain, own = 1.0, jax.random.fold_in(key, 6)
    for dim, shards_of in shards:
        heights = jnp.exp(jax.random.uniform(jax.random.fold_in(own, dim), (shards_of,), jnp.float32, least / len(shards), top_value / len(shards)))
        gain = gain * jnp.repeat(heights, shape[dim] // shards_of).reshape([-1 if axis == dim else 1 for axis in range(len(shape))])
    return gain


def split_up(number_of, total, most, slope):
    portions = [(1 << 20) // math.isqrt(grade ** slope) + 1 for grade in range(2, number_of + 1)]
    rest, counts = total - most - (number_of - 1), [1] * (number_of - 1)
    while rest > 0:
        movable = [i for i in range(number_of - 1) if counts[i] < most]
        whole, left = sum([portions[i] for i in movable]), rest
        for i in movable:
            addition = min(most - counts[i], max(1, left * portions[i] // whole), rest)
            counts[i] = counts[i] + addition
            rest = rest - addition
    return np.array([most] + counts)


def ragged(stream_key, count, total, reach, slope):
    if count == 2:
        one = jax.random.randint(stream_key, (), max(1, total - reach), min(reach, total - 1) + 1)
        return jnp.stack([one, total - one])
    tallies = jnp.asarray(split_up(count, total, reach, slope), jnp.int32)
    couples = (count - 1) // 2
    donor, receiver = tallies[1:1 + 2 * couples:2], tallies[2:2 + 2 * couples:2]
    slack = jnp.minimum(donor - 1, reach - receiver)
    shifted = jax.random.randint(jax.random.fold_in(stream_key, 1), (couples,), 0, 1 << 20) % (slack + 1)
    tallies = tallies.at[1:1 + 2 * couples:2].set(donor - shifted).at[2:2 + 2 * couples:2].set(receiver + shifted)
    return tallies[jax.random.permutation(jax.random.fold_in(stream_key, 2), count)]


def bell_draw(stream_key, shape, deviation, limit, cuts=(), held_as=jnp.bfloat16):
    entries = deviation * jax.random.normal(stream_key, shape, jnp.float32)
    if cuts:
        entries = entries * shard_levels(stream_key, shape, cuts, -0.22, 0.18)
    return jnp.clip(entries, -limit, limit).astype(held_as)


def setup_inputs(seed: int = 0) -> dict:
    streams_of = jax.random.split(jax.random.key(seed), 14)
    queries = draw_queries(jax.random.fold_in(streams_of[13], 71), 0)
    keys = draw_keys(jax.random.fold_in(streams_of[13], 71), 0)
    values = bell_draw(streams_of[2], (TOKENS, KV_W), 3.0, 18.0, ((0, 16), (1, 2)))
    doc_ids = jnp.searchsorted(jnp.cumsum(ragged(streams_of[3], DOCS, TOKENS, TOKENS // 2, 0)), jnp.arange(TOKENS), side="right").astype(jnp.int32)
    sinks = jnp.clip(4.0 * jax.random.uniform(streams_of[4], (A_HEADS,), jnp.float32) ** shard_levels(streams_of[4], (A_HEADS,), ((0, 2),), -0.2, 0.2), 0.0, 4.0)
    residual = draw_residual(jax.random.fold_in(streams_of[13], 71), 0)
    out_weight = bell_draw(streams_of[6], (A_Q, D), A_Q ** -0.5, 0.1875, ((0, 2),))
    norm_gain = jnp.clip(1.0 + 0.18 * jax.random.normal(streams_of[7], (D,), jnp.float32), 0.1, 1.9)
    w_gate = bell_draw(streams_of[8], (D, FF), D ** -0.5, 0.125, ((0, 16), (1, 2)))
    w_value = bell_draw(streams_of[9], (D, FF), D ** -0.5, 0.125, ((0, 16), (1, 2)))
    conv_gate = bell_draw(streams_of[10], (3, FF), 3 ** -0.5, 3.5, ((1, 2),), jnp.float32)
    conv_value = bell_draw(streams_of[11], (3, FF), 3 ** -0.5, 3.5, ((1, 2),), jnp.float32)
    w_down = bell_draw(streams_of[12], (FF, D), FF ** -0.5, 0.078125, ((0, 2), (1, 16)))
    return dict(queries=queries, keys=keys, values=values, doc_ids=doc_ids, sinks=sinks, residual=residual, out_weight=out_weight, norm_gain=norm_gain, w_gate=w_gate, w_value=w_value, conv_gate=conv_gate, conv_value=conv_value, w_down=w_down)


def attend(query_rows, key_ext, value_ext, doc_rows, doc_ext, sinks):
    row_count = query_rows.shape[0]
    block_count = row_count // WINDOW
    kv_heads = key_ext.shape[1] // HEAD_DIM
    group_size = query_rows.shape[1] // (kv_heads * HEAD_DIM)

    def band(t):
        lower = t[:row_count].reshape((block_count, WINDOW) + t.shape[1:])
        upper = t[WINDOW:].reshape((block_count, WINDOW) + t.shape[1:])
        return jnp.concatenate([lower, upper], axis=1)
    query_band = query_rows.astype(jnp.float32).reshape(block_count, WINDOW, kv_heads, group_size, HEAD_DIM)
    key_band = band(key_ext).astype(jnp.float32).reshape(block_count, 2 * WINDOW, kv_heads, HEAD_DIM)
    value_band = band(value_ext).astype(jnp.float32).reshape(block_count, 2 * WINDOW, kv_heads, HEAD_DIM)
    doc_band = band(doc_ext)
    distance = jnp.arange(WINDOW)[:, None] + WINDOW - jnp.arange(2 * WINDOW)[None, :]
    in_window = (distance >= 0) & (distance < WINDOW)
    same_doc = doc_rows.reshape(block_count, WINDOW)[:, :, None] == doc_band[:, None, :]
    keep_mask = in_window[None] & same_doc
    scores = jnp.einsum('nqhgd,nkhd->nhgqk', query_band, key_band) * HEAD_DIM ** (-0.5)
    scores = jnp.where(keep_mask[:, None, None], scores, -jnp.inf)
    sink_logit = sinks.astype(jnp.float32).reshape(kv_heads, group_size)[None, :, :, None, None]
    peak = jnp.maximum(lax.optimization_barrier(jnp.max(scores, axis=-1, keepdims=True)), sink_logit)
    expd = jnp.exp(scores - peak)
    probs = (expd / (lax.optimization_barrier(jnp.sum(expd, axis=-1, keepdims=True)) + jnp.exp(sink_logit - peak))).astype(jnp.bfloat16)
    mixed = jnp.einsum('nhgqk,nkhd->nqhgd', probs.astype(jnp.float32), value_band)
    return mixed.astype(jnp.bfloat16).reshape(row_count, -1)

def convolve(ext_rows, doc_ext, taps):
    center = doc_ext[2:]
    same_one = (doc_ext[1:-1] == center)[:, None]
    same_two = (doc_ext[:-2] == center)[:, None]
    ext32 = ext_rows.astype(jnp.float32)
    result = taps[2] * ext32[2:]
    result = result + jnp.where(same_one, taps[1] * ext32[1:-1], 0.0)
    return result + jnp.where(same_two, taps[0] * ext32[:-2], 0.0)

def reference(queries, keys, values, doc_ids, sinks, residual, out_weight, norm_gain, w_gate, w_value, conv_gate, conv_value, w_down):
    docs_plus = doc_ids + 1
    key_pad = jnp.concatenate([jnp.zeros((WINDOW, KV_W), jnp.bfloat16), keys], axis=0)
    value_pad = jnp.concatenate([jnp.zeros((WINDOW, KV_W), jnp.bfloat16), values], axis=0)
    doc_pad = jnp.concatenate([jnp.zeros((WINDOW,), jnp.int32), docs_plus], axis=0)

    def attend_shard(index):
        start = (index * TOK_SP).astype(jnp.int32)
        return attend(lax.dynamic_slice_in_dim(queries, start, TOK_SP, 0), lax.dynamic_slice_in_dim(key_pad, start, TOK_SP + WINDOW, 0), lax.dynamic_slice_in_dim(value_pad, start, TOK_SP + WINDOW, 0), lax.dynamic_slice_in_dim(docs_plus, start, TOK_SP, 0), lax.dynamic_slice_in_dim(doc_pad, start, TOK_SP + WINDOW, 0), sinks)
    shard_ids = jnp.arange(N_SP, dtype=jnp.int32)
    attn = lax.map(attend_shard, shard_ids).reshape(TOKENS, A_Q)
    proj = jnp.dot(attn, out_weight, preferred_element_type=jnp.float32)
    mid = (residual.astype(jnp.float32) + proj).astype(jnp.bfloat16)
    mid32 = mid.astype(jnp.float32)
    normed = (mid32 * lax.rsqrt(lax.optimization_barrier(jnp.mean(mid32 * mid32, axis=-1, keepdims=True)) + 1e-06) * norm_gain).astype(jnp.bfloat16)
    normed_pad = jnp.concatenate([jnp.zeros((2, D), jnp.bfloat16), normed], axis=0)
    doc_two = jnp.concatenate([jnp.zeros((2,), jnp.int32), docs_plus], axis=0)

    def mlp_shard(index):
        start = (index * TOK_SP).astype(jnp.int32)
        rows_ext = lax.dynamic_slice_in_dim(normed_pad, start, TOK_SP + 2, 0)
        doc_ext = lax.dynamic_slice_in_dim(doc_two, start, TOK_SP + 2, 0)
        gate_pre = jnp.dot(rows_ext, w_gate, preferred_element_type=jnp.float32).astype(jnp.bfloat16)
        value_pre = jnp.dot(rows_ext, w_value, preferred_element_type=jnp.float32).astype(jnp.bfloat16)
        gate_conv = convolve(gate_pre, doc_ext, conv_gate)
        value_conv = convolve(value_pre, doc_ext, conv_value)
        hidden = (jax.nn.silu(gate_conv) * value_conv).astype(jnp.bfloat16)
        return jnp.dot(hidden, w_down, preferred_element_type=jnp.float32)
    mlp = lax.map(mlp_shard, shard_ids).reshape(TOKENS, D)
    return (mid32 + mlp).astype(jnp.bfloat16)
```

```python
import jax
import jax.numpy as jnp
import numpy as np
from jax import lax
from jax.experimental import pallas as pl
from jax.experimental.pallas import tpu as pltpu
from jax.sharding import PartitionSpec as P

HEAD_DIM = 64
WINDOW = 128
LANES = 128
HALO = 16
COLS = 256
VMEM_BYTES = 60 * 1024 * 1024


def shifted(shard, axis, by):
    size = lax.axis_size(axis)
    pairs = [(i, i + by) for i in range(size) if 0 <= i + by < size]
    return lax.ppermute(shard, axis, pairs)


def attend(query_rows, key_ext, value_ext, doc_rows, doc_ext, sinks):
    row_count = query_rows.shape[0]
    block_count = row_count // WINDOW
    kv_heads = key_ext.shape[1] // HEAD_DIM
    group_size = query_rows.shape[1] // (kv_heads * HEAD_DIM)

    def band(t):
        lower = t[:row_count].reshape((block_count, WINDOW) + t.shape[1:])
        upper = t[WINDOW:].reshape((block_count, WINDOW) + t.shape[1:])
        return jnp.concatenate([lower, upper], axis=1)

    query_band = query_rows.reshape(block_count, WINDOW, kv_heads, group_size, HEAD_DIM)
    key_band = band(key_ext).reshape(block_count, 2 * WINDOW, kv_heads, HEAD_DIM)
    value_band = band(value_ext).reshape(block_count, 2 * WINDOW, kv_heads, HEAD_DIM)
    doc_band = band(doc_ext)
    distance = jnp.arange(WINDOW)[:, None] + WINDOW - jnp.arange(2 * WINDOW)[None, :]
    in_window = (distance >= 0) & (distance < WINDOW)
    same_doc = doc_rows.reshape(block_count, WINDOW)[:, :, None] == doc_band[:, None, :]
    keep_mask = in_window[None] & same_doc
    scores = jnp.einsum(
        "nqhgd,nkhd->nhgqk", query_band, key_band, preferred_element_type=jnp.float32
    ) * HEAD_DIM ** (-0.5)
    scores = jnp.where(keep_mask[:, None, None], scores, -jnp.inf)
    sink_logit = sinks.reshape(kv_heads, group_size)[None, :, :, None, None]
    peak = jnp.maximum(jnp.max(scores, axis=-1, keepdims=True), sink_logit)
    expd = jnp.exp(scores - peak)
    probs = (expd / (jnp.sum(expd, axis=-1, keepdims=True) + jnp.exp(sink_logit - peak))).astype(
        jnp.bfloat16
    )
    mixed = jnp.einsum("nhgqk,nkhd->nqhgd", probs, value_band, preferred_element_type=jnp.float32)
    return mixed.astype(jnp.bfloat16).reshape(row_count, -1)


def convolve(ext_rows, doc_ext, taps):
    center = doc_ext[2:]
    same_one = (doc_ext[1:-1] == center)[:, None]
    same_two = (doc_ext[:-2] == center)[:, None]
    ext32 = ext_rows.astype(jnp.float32)
    result = taps[2] * ext32[2:]
    result = result + jnp.where(same_one, taps[1] * ext32[1:-1], 0.0)
    return result + jnp.where(same_two, taps[0] * ext32[:-2], 0.0)


def from_ahead(shard, axis, by):
    size = lax.axis_size(axis)
    return lax.ppermute(shard, axis, [((i + by) % size, i) for i in range(size)])


def peer_weight(shard, by):
    half = shard.shape[0] // 2
    sp_size = lax.axis_size("sp")
    if sp_size % 2:
        got = from_ahead(shard, "tp", by)
        return ((0, got[:half]), (half, got[half:]))
    parity = lax.axis_index("sp") % 2
    mine = from_ahead(lax.dynamic_slice_in_dim(shard, parity * half, half, 0), "tp", by)
    other = lax.ppermute(mine, "sp", [(i, i ^ 1) for i in range(sp_size)])
    return ((parity * half, mine), ((1 - parity) * half, other))


def chip_ring(sp_size):
    chips = sp_size // 2
    return list(range(0, chips, 2)) + list(range(1, chips, 2))[::-1]


def ring_steps(shard, ring):
    count = len(ring)
    hops = [(ring[p], ring[(p + 1) % count]) for p in range(count)]
    ahead = [(2 * a + k, 2 * b + k) for a, b in hops for k in (0, 1)]
    behind = [(b, a) for a, b in ahead]
    got, up, down = [shard], shard, shard
    for _ in range((count - 1) // 2):
        up = lax.ppermute(up, "sp", ahead)
        down = lax.ppermute(down, "sp", behind)
        got += [up, down]
    half = shard.shape[0] // 2
    got.append(
        jnp.concatenate(
            [lax.ppermute(up[:half], "sp", ahead), lax.ppermute(down[half:], "sp", behind)], axis=0
        )
    )
    return got


def with_partner(got):
    swap = [(i, i ^ 1) for i in range(lax.axis_size("sp"))]
    return [t for g in got for t in (g, lax.ppermute(g, "sp", swap))]


def slab_owners(sp_size):
    ring = chip_ring(sp_size)
    count = len(ring)
    table = np.zeros((sp_size, sp_size), np.int32)
    for p in range(count):
        offsets = [0]
        for step in range(1, (count - 1) // 2 + 1):
            offsets += [-step, step]
        offsets.append(count // 2)
        for k in (0, 1):
            chips = [ring[(p + o) % count] for o in offsets]
            table[2 * ring[p] + k] = [2 * c + (k ^ other) for c in chips for other in (0, 1)]
    return table


def up_block(x_rows, masks, owners, slabs, conv_gate, conv_value):
    rows, depth = x_rows.shape
    out_rows = rows - HALO
    channels = conv_gate.shape[1]
    blocks = channels // COLS
    count = len(slabs)
    part = slabs[0].shape[0]

    def kernel(owner_ref, x_ref, one_ref, two_ref, gate_taps, value_taps, *refs):
        gate_refs, value_refs = refs[:count], refs[count : 2 * count]
        out_ref, x_turned = refs[2 * count :]

        @pl.when(pl.program_id(0) == 0)
        def _():
            for i in range(count):
                at = pl.multiple_of(owner_ref[i] * part, LANES)
                x_turned[:, i * part : (i + 1) * part] = x_ref[:, pl.ds(at, part)]

        x = x_turned[...]
        one = jnp.concatenate([one_ref[...]] * (COLS // LANES), axis=1)
        two = jnp.concatenate([two_ref[...]] * (COLS // LANES), axis=1)

        def conv(weight_refs, taps):
            weights = jnp.concatenate([r[...] for r in weight_refs], axis=0)
            pre = jnp.dot(x, weights, preferred_element_type=jnp.float32)
            pre = pre.astype(jnp.bfloat16).astype(jnp.float32)
            back_one = pltpu.roll(pre, 1, 0)[HALO:]
            back_two = pltpu.roll(pre, 2, 0)[HALO:]
            result = taps[2:3] * pre[HALO:] + one * (taps[1:2] * back_one)
            return result + two * (taps[0:1] * back_two)

        gate = conv(gate_refs, gate_taps[...])
        value = conv(value_refs, value_taps[...])
        out_ref[...] = (gate / (1.0 + jnp.exp(-gate)) * value).astype(jnp.bfloat16)

    whole = lambda shape: pl.BlockSpec(shape, lambda j, o: (0, 0))
    column = lambda rows, first: pl.BlockSpec((rows, COLS), lambda j, o: (0, first + j))
    return pl.pallas_call(
        kernel,
        grid_spec=pltpu.PrefetchScalarGridSpec(
            num_scalar_prefetch=1,
            grid=(blocks,),
            in_specs=[whole(x_rows.shape), whole(masks[0].shape), whole(masks[1].shape)]
            + [column(3, 0), column(3, 0)]
            + [column(part, 0)] * count
            + [column(part, blocks)] * count,
            out_specs=column(out_rows, 0),
            scratch_shapes=[pltpu.VMEM((rows, depth), jnp.bfloat16)],
        ),
        out_shape=jax.ShapeDtypeStruct((out_rows, channels), jnp.bfloat16),
        compiler_params=pltpu.CompilerParams(vmem_limit_bytes=VMEM_BYTES),
    )(owners, x_rows, *masks, conv_gate, conv_value, *slabs, *slabs)


def down_block(hidden, slabs, dtype):
    rows, channels = hidden.shape
    tile = min(rows, 256)
    count = len(slabs)
    part = slabs[0].shape[1]

    def kernel(hidden_ref, *refs):
        out_ref = refs[count]
        x = hidden_ref[...]
        for i in range(0, count, 2):
            weights = jnp.concatenate([refs[i][...], refs[i + 1][...]], axis=1)
            terms = jnp.dot(x, weights, preferred_element_type=jnp.float32)
            out_ref[:, i * part : (i + 2) * part] = terms.astype(dtype)

    return pl.pallas_call(
        kernel,
        grid=(rows // tile,),
        in_specs=[pl.BlockSpec((tile, channels), lambda m: (m, 0))]
        + [pl.BlockSpec(slabs[0].shape, lambda m: (0, 0))] * count,
        out_specs=pl.BlockSpec((tile, count * part), lambda m: (m, 0)),
        out_shape=jax.ShapeDtypeStruct((rows, count * part), dtype),
        compiler_params=pltpu.CompilerParams(vmem_limit_bytes=VMEM_BYTES),
    )(hidden, *slabs)


def finish(owners, mid, own, received):
    rows, width = mid.shape
    tile = min(rows, 128)
    part = width // owners.shape[0]

    def kernel(owner_ref, mid_ref, own_ref, *refs):
        out_ref = refs[-1]
        for i in range(owners.shape[0]):
            cols = slice(i * part, (i + 1) * part)
            at = pl.multiple_of(owner_ref[i] * part, LANES)
            total = mid_ref[:, pl.ds(at, part)].astype(jnp.float32) + own_ref[:, cols]
            for (start, _), ref in zip(spans, refs):
                if start <= i * part < start + ref.shape[1]:
                    inner = slice(i * part - start, (i + 1) * part - start)
                    total = total + ref[:, inner].astype(jnp.float32)
            out_ref[:, pl.ds(at, part)] = total.astype(jnp.bfloat16)

    spans = [(start, t.shape[1]) for start, t in received]
    row_block = lambda cols: pl.BlockSpec((tile, cols), lambda m, o: (m, 0))
    return pl.pallas_call(
        kernel,
        grid_spec=pltpu.PrefetchScalarGridSpec(
            num_scalar_prefetch=1,
            grid=(rows // tile,),
            in_specs=[row_block(width), row_block(width)]
            + [row_block(t.shape[1]) for _, t in received],
            out_specs=row_block(width),
        ),
        out_shape=jax.ShapeDtypeStruct(mid.shape, jnp.bfloat16),
        compiler_params=pltpu.CompilerParams(vmem_limit_bytes=VMEM_BYTES),
    )(owners, mid, own, *[t for _, t in received])


def per_device(
    queries,
    keys,
    values,
    doc_ids,
    sinks,
    residual,
    out_weight,
    norm_gain,
    w_gate,
    w_value,
    conv_gate,
    conv_value,
    w_down,
):
    tp_size = lax.axis_size("tp")
    tp_index = lax.axis_index("tp")
    row_count = queries.shape[0]
    own_rows = row_count // tp_size

    sp_size = lax.axis_size("sp")
    by_ring = (
        sp_size % 4 == 0
        and w_gate.shape[0] % LANES == 0
        and w_down.shape[1] % LANES == 0
        and w_gate.shape[1] % COLS == 0
        and own_rows % COLS == 0
    )
    if by_ring:
        ring = chip_ring(sp_size)
        up_got = ring_steps(jnp.concatenate([w_gate, w_value], axis=1), ring)
        up_slabs = with_partner(up_got)
        w_down, _, _ = lax.optimization_barrier((w_down, up_got[-3], up_got[-2]))
        down_slabs = with_partner(ring_steps(w_down, ring))
        owners = lax.dynamic_index_in_dim(
            jnp.asarray(slab_owners(sp_size)), lax.axis_index("sp"), 0, keepdims=False
        )
    else:
        gate_all = lax.all_gather(w_gate, "sp", axis=0, tiled=True)
        value_all = lax.all_gather(w_value, "sp", axis=0, tiled=True)
        down_all = lax.all_gather(w_down, "sp", axis=1, tiled=True)
    peers = [peer_weight(out_weight, by) for by in range(1, tp_size)]

    docs_plus = doc_ids + 1
    width = keys.shape[1]
    kv = jnp.concatenate([keys, values], axis=1)
    prev_kv, prev_docs = shifted((kv[-WINDOW:], docs_plus[-WINDOW:]), "sp", 1)
    kv_ext = jnp.concatenate([prev_kv, kv], axis=0)
    doc_ext = jnp.concatenate([prev_docs, docs_plus], axis=0)
    head_out = attend(queries, kv_ext[:, :width], kv_ext[:, width:], docs_plus, doc_ext, sinks)

    def rows_of(t, index):
        return lax.dynamic_slice_in_dim(t, index * own_rows, own_rows, 0)

    proj = jnp.dot(rows_of(head_out, tp_index), out_weight, preferred_element_type=jnp.float32)
    for by in range(1, tp_size):
        got = from_ahead(rows_of(head_out, (tp_index - by) % tp_size), "tp", by)
        for start, rows in peers[by - 1]:
            cols = lax.dynamic_slice_in_dim(got, start, rows.shape[0], 1)
            proj = proj + jnp.dot(cols, rows, preferred_element_type=jnp.float32)
    mid32 = (residual.astype(jnp.float32) + proj).astype(jnp.bfloat16).astype(jnp.float32)
    normed = (
        mid32 * lax.rsqrt(jnp.mean(mid32 * mid32, axis=-1, keepdims=True) + 1e-06) * norm_gain
    ).astype(jnp.bfloat16)
    if by_ring:
        ext = jnp.zeros((HALO + row_count, normed.shape[1]), normed.dtype)
        for by in range(tp_size):
            block = from_ahead(normed, "tp", by) if by else normed
            at = HALO + (tp_index + by) % tp_size * own_rows
            ext = lax.dynamic_update_slice_in_dim(ext, block, at, 0)
        ext = lax.dynamic_update_slice_in_dim(ext, shifted(ext[-2:], "sp", 1), HALO - 2, 0)
        conv_docs = jnp.concatenate([prev_docs[-2:], docs_plus], axis=0)
        same = [
            jnp.broadcast_to(
                (conv_docs[2 - back : 2 - back + row_count] == docs_plus)[:, None],
                (row_count, LANES),
            ).astype(jnp.float32)
            for back in (1, 2)
        ]

        def hidden_of(index):
            x_rows = lax.dynamic_slice_in_dim(ext, index * own_rows, HALO + own_rows, 0)
            masks = [rows_of(m, index) for m in same]
            return up_block(x_rows, masks, owners, up_slabs, conv_gate, conv_value)

        early = len(down_slabs) - 6
        received = []
        for by in range(1, tp_size):
            hidden = hidden_of((tp_index - by) % tp_size)
            first = down_block(hidden, down_slabs[:early], jnp.bfloat16)
            received.append((0, from_ahead(first, "tp", by)))
            second = down_block(hidden, down_slabs[early:], jnp.bfloat16)
            received.append((early * w_down.shape[1], from_ahead(second, "tp", by)))
        own = down_block(hidden_of(tp_index), down_slabs, jnp.float32)
        return finish(owners, mid32.astype(jnp.bfloat16), own, received)

    whole = jnp.zeros((row_count, normed.shape[1]), normed.dtype)
    for by in range(tp_size):
        block = from_ahead(normed, "tp", by) if by else normed
        at = (tp_index + by) % tp_size * own_rows
        whole = lax.dynamic_update_slice_in_dim(whole, block, at, 0)

    gate_pre = jnp.dot(whole, gate_all, preferred_element_type=jnp.float32).astype(jnp.bfloat16)
    value_pre = jnp.dot(whole, value_all, preferred_element_type=jnp.float32).astype(jnp.bfloat16)
    prev_gate, prev_value = shifted((gate_pre[-2:], value_pre[-2:]), "sp", 1)
    conv_docs = jnp.concatenate([prev_docs[-2:], docs_plus], axis=0)
    gate_conv = convolve(jnp.concatenate([prev_gate, gate_pre], axis=0), conv_docs, conv_gate)
    value_conv = convolve(jnp.concatenate([prev_value, value_pre], axis=0), conv_docs, conv_value)
    hidden = (jax.nn.silu(gate_conv) * value_conv).astype(jnp.bfloat16)
    hidden, down_all = lax.optimization_barrier((hidden, down_all))

    def terms_of(index):
        return jnp.dot(rows_of(hidden, index), down_all, preferred_element_type=jnp.float32)

    total = mid32
    for by in range(1, tp_size):
        terms = terms_of((tp_index - by) % tp_size).astype(jnp.bfloat16)
        total = total + from_ahead(terms, "tp", by).astype(jnp.float32)
    return (total + terms_of(tp_index)).astype(jnp.bfloat16)


def solution(mesh):
    return jax.shard_map(
        per_device,
        mesh=mesh,
        in_specs=(
            P("sp", "tp"),
            P("sp", "tp"),
            P("sp", "tp"),
            P("sp"),
            P("tp"),
            P(("sp", "tp"), None),
            P("tp", None),
            P(),
            P("sp", "tp"),
            P("sp", "tp"),
            P(None, "tp"),
            P(None, "tp"),
            P("tp", "sp"),
        ),
        out_specs=P(("sp", "tp"), None),
        check_vma=False,
    )
```
